32 devices in a mesh: sp: 8 (over z, x), dp: 4 (over y, core).
Axes of the slice: x: 2, y: 2, z: 4, core: 2. Of those that a mesh axis runs over, the one named last changes fastest.
Arguments:
- inputs: bfloat16 [4, 2048, 2048], P('dp', 'sp'), may hold values from -6 to 6
- up_pre: bfloat16 [4, 2048, 1024], P('dp', 'sp'), may hold values from -6 to 6
- gate_pre: bfloat16 [4, 2048, 1024], P('dp', 'sp'), may hold values from -6 to 6
- cotangent: bfloat16 [4, 2048, 1024], P('dp', 'sp'), may hold values from -6 to 6
- norm_gain: float32 [1024], replicated, may hold values from 0.1 to 1.9
- up_weight: bfloat16 [2048, 1024], P('dp'), may hold values from -0.125 to 0.125
- gate_weight: bfloat16 [2048, 1024], P('dp'), may hold values from -0.125 to 0.125
- mix_weight: bfloat16 [8, 512, 512], replicated, may hold values from -0.375 to 0.375
Outputs:
- input_grad: bfloat16 [4, 2048, 2048], P('dp', 'sp')
- up_weight_grad: float32 [2048, 1024], P('dp')
- gate_weight_grad: float32 [2048, 1024], P('dp')
The draws below stay inside these ranges and needn't reach their ends.
All inputs are finite; a program needn't handle non-finite values.
Results may differ from the reference program's by a relative error of at most 0.0064.
Values may be sent and summed in bfloat16 or wider, within the bound.
A program may use at most 128 MiB of HBM per device.

```python
import math
import jax
import jax.numpy as jnp
from jax import lax

MODEL = 2048
GROUPS = 8
GROUP_CH = 128
SPAN = 512
SEG = 64
GATED = 1024
LENGTH = 2048
BATCH = 4


def levels(stream_key, dims, pieces, smallest, high):
    loudness = 1.0
    for axis_at, parts in pieces:
        draws = jax.random.uniform(jax.random.fold_in(jax.random.fold_in(stream_key, 6), axis_at), (parts,), jnp.float32, smallest / len(pieces), high / len(pieces))
        loudness = loudness * jnp.repeat(jnp.exp(draws), dims[axis_at] // parts).reshape((-1,) + (1,) * (len(dims) - 1 - axis_at))
    return loudness


def noise(own_key, shape, deviation, reach, split=(), dtype=jnp.bfloat16):
    entries = deviation * jax.random.normal(own_key, shape, jnp.float32)
    if split:
        entries = entries * levels(own_key, shape, split, -0.22, 0.18)
    return jnp.clip(entries, -reach, reach).astype(dtype)


def setup_inputs(seed: int = 0) -> dict:
    key_list = jax.random.split(jax.random.key(seed), 9)
    inputs = noise(key_list[0], (BATCH, LENGTH, MODEL), 1.0, 6.0, ((0, 4), (1, 8)))
    up_pre = noise(key_list[1], (BATCH, LENGTH, GATED), 1.0, 6.0, ((0, 4), (1, 8)))
    gate_pre = noise(key_list[2], (BATCH, LENGTH, GATED), 1.0, 6.0, ((0, 4), (1, 8)))
    cotangent = noise(key_list[3], (BATCH, LENGTH, GATED), 1.0, 6.0, ((0, 4), (1, 8)))
    norm_gain = jnp.clip(1.0 + 0.18 * jax.random.normal(key_list[4], (GATED,), jnp.float32), 0.1, 1.9)
    up_weight = noise(key_list[5], (MODEL, GATED), MODEL ** -0.5, 0.125, ((0, 4),))
    gate_weight = noise(key_list[6], (MODEL, GATED), MODEL ** -0.5, 0.125, ((0, 4),))
    mix_weight = noise(key_list[7], (GROUPS, SPAN, SPAN), (SPAN // 2) ** -0.5, 0.375)
    return dict(inputs=inputs, up_pre=up_pre, gate_pre=gate_pre, cotangent=cotangent, norm_gain=norm_gain, up_weight=up_weight, gate_weight=gate_weight, mix_weight=mix_weight)


norm_eps = 1e-05
grad_scale = 1.0 / 256.0
root_half = 1.0 / math.sqrt(2.0)
root_twopi = 1.0 / math.sqrt(2.0 * math.pi)

def gelu_value(preact):
    return 0.5 * preact * (1.0 + lax.erf(preact * root_half))

def gelu_slope(preact):
    return 0.5 * (1.0 + lax.erf(preact * root_half)) + preact * jnp.exp(-0.5 * preact * preact) * root_twopi

def span_mask():
    segment = jnp.arange(SPAN) // SEG
    return segment[None, :] <= segment[:, None]

def reference(inputs, up_pre, gate_pre, cotangent, norm_gain, up_weight, gate_weight, mix_weight):
    up_float = up_pre.astype(jnp.float32)
    gate_float = gate_pre.astype(jnp.float32)
    grad_float = cotangent.astype(jnp.float32)
    gated_act = gelu_value(gate_float)
    centered = gated_act - lax.optimization_barrier(jnp.mean(gated_act, axis=-1, keepdims=True))
    inverse_std = lax.rsqrt(lax.optimization_barrier(jnp.mean(centered * centered, axis=-1, keepdims=True)) + norm_eps)
    normed = centered * inverse_std
    mixer_in = (normed * norm_gain).astype(jnp.bfloat16)
    mixer_grad = (grad_float * gelu_value(up_float)).astype(jnp.bfloat16)
    masked = jnp.where(span_mask()[None], mix_weight, jnp.zeros_like(mix_weight)).astype(jnp.float32)
    block_count = LENGTH // SPAN
    block_shape = (BATCH, block_count, SPAN, GROUPS, GROUP_CH)
    input_blocks = mixer_in.astype(jnp.float32).reshape(block_shape)
    grad_blocks = mixer_grad.astype(jnp.float32).reshape(block_shape)
    spatial = jnp.einsum('gts,bnsgc->bntgc', masked, input_blocks).astype(jnp.bfloat16)
    spatial = spatial.reshape(BATCH, LENGTH, GATED)
    normed_back = jnp.einsum('gts,bntgc->bnsgc', masked, grad_blocks).astype(jnp.bfloat16)
    normed_back = normed_back.reshape(BATCH, LENGTH, GATED)
    up_pre_grad = (grad_float * spatial.astype(jnp.float32) * gelu_slope(up_float)).astype(jnp.bfloat16)
    scaled = normed_back.astype(jnp.float32) * norm_gain
    gated_grad = inverse_std * (scaled - lax.optimization_barrier(jnp.mean(scaled, axis=-1, keepdims=True)) - normed * lax.optimization_barrier(jnp.mean(scaled * normed, axis=-1, keepdims=True)))
    gate_pre_grad = (gated_grad * gelu_slope(gate_float)).astype(jnp.bfloat16)
    flat_up = up_pre_grad.reshape(-1, GATED)
    flat_gate = gate_pre_grad.reshape(-1, GATED)
    flat_inputs = inputs.reshape(-1, MODEL)
    input_grad = jnp.dot(flat_up, up_weight.T, preferred_element_type=jnp.float32) + jnp.dot(flat_gate, gate_weight.T, preferred_element_type=jnp.float32)
    input_grad = input_grad.astype(jnp.bfloat16).reshape(BATCH, LENGTH, MODEL)
    up_weight_grad = jnp.dot(flat_inputs.T, flat_up, preferred_element_type=jnp.float32) * grad_scale
    gate_weight_grad = jnp.dot(flat_inputs.T, flat_gate, preferred_element_type=jnp.float32) * grad_scale
    return (input_grad, up_weight_grad, gate_weight_grad)
```

```python
import math

import jax
import jax.numpy as jnp
from jax import lax
from jax.sharding import PartitionSpec as P

GROUP_CH = 128
SPAN = 512
SEG = 64


norm_eps = 1e-05
grad_scale = 1.0 / 256.0
root_half = 1.0 / math.sqrt(2.0)
root_twopi = 1.0 / math.sqrt(2.0 * math.pi)


def gelu_value(preact):
    return 0.5 * preact * (1.0 + lax.erf(preact * root_half))


def gelu_slope(preact):
    return (
        0.5 * (1.0 + lax.erf(preact * root_half))
        + preact * jnp.exp(-0.5 * preact * preact) * root_twopi
    )


def contract(first_op, second_op, first_dim, second_dim):
    return lax.dot_general(
        first_op,
        second_op,
        (((first_dim,), (second_dim,)), ((), ())),
        preferred_element_type=jnp.float32,
    )


def on_device(inputs, up_pre, gate_pre, cotangent, norm_gain, up_weight, gate_weight, mix_weight):
    sequences, own_rows, gated_width = cotangent.shape
    model_width = inputs.shape[2]
    sp_count = lax.axis_size("sp")
    assert sequences == 1 and own_rows * 2 == SPAN
    groups = gated_width // GROUP_CH
    input_columns = lax.all_to_all(inputs[0], "dp", split_axis=1, concat_axis=0, tiled=True)
    up_float = up_pre[0].astype(jnp.float32)
    gate_float = gate_pre[0].astype(jnp.float32)
    grad_float = cotangent[0].astype(jnp.float32)
    gated_act = gelu_value(gate_float)
    centered = gated_act - jnp.mean(gated_act, axis=-1, keepdims=True)
    inverse_std = lax.rsqrt(jnp.mean(centered * centered, axis=-1, keepdims=True) + norm_eps)
    normed = centered * inverse_std
    mixer_in = (normed * norm_gain).astype(jnp.bfloat16)
    mixer_grad = (grad_float * gelu_value(up_float)).astype(jnp.bfloat16)
    half = lax.axis_index("sp") % 2
    arrived = lax.ppermute(
        jnp.where(half == 0, mixer_in, mixer_grad), "sp", [(i, i ^ 1) for i in range(sp_count)]
    )
    segment = jnp.arange(own_rows) // SEG
    own_block = lax.dynamic_slice(
        mix_weight, (0, half * own_rows, half * own_rows), (groups, own_rows, own_rows)
    )
    own_block = jnp.where(
        segment[None, :] <= segment[:, None], own_block, jnp.zeros_like(own_block)
    )
    cross_block = mix_weight[:, own_rows:, :own_rows]
    cross_block = jnp.where(half == 0, cross_block.transpose(0, 2, 1), cross_block)
    shape = (own_rows, groups, GROUP_CH)
    own_in = mixer_in.reshape(shape)
    own_grad = mixer_grad.reshape(shape)
    f32 = jnp.float32
    cross = jnp.einsum("gts,sgc->tgc", cross_block, arrived.reshape(shape), preferred_element_type=f32)
    spatial = jnp.einsum("gts,sgc->tgc", own_block, own_in, preferred_element_type=f32)
    back = jnp.einsum("gts,tgc->sgc", own_block, own_grad, preferred_element_type=f32)
    flat = (own_rows, gated_width)
    spatial = (spatial + jnp.where(half == 0, 0.0, cross)).astype(jnp.bfloat16).reshape(flat)
    back = (back + jnp.where(half == 0, cross, 0.0)).astype(jnp.bfloat16).reshape(flat)
    up_pre_grad = (grad_float * spatial.astype(f32) * gelu_slope(up_float)).astype(jnp.bfloat16)
    scaled = back.astype(f32) * norm_gain
    gated_grad = inverse_std * (
        scaled
        - jnp.mean(scaled, axis=-1, keepdims=True)
        - normed * jnp.mean(scaled * normed, axis=-1, keepdims=True)
    )
    gate_pre_grad = (gated_grad * gelu_slope(gate_float)).astype(jnp.bfloat16)
    both_grads = jnp.concatenate([up_pre_grad, gate_pre_grad], axis=1)
    all_grads = lax.all_gather(both_grads, "dp", axis=0, tiled=True)
    weight_part = contract(input_columns, all_grads, 0, 0).astype(jnp.bfloat16)
    own_part = lax.psum_scatter(weight_part, "sp", scatter_dimension=0, tiled=True)
    weight_rows = lax.all_gather(own_part, "sp", axis=0, tiled=True).astype(f32)
    both_weights = jnp.concatenate([up_weight, gate_weight], axis=1)
    result_part = contract(all_grads, both_weights, 1, 1).astype(jnp.bfloat16)
    input_grad = lax.all_to_all(result_part, "dp", split_axis=0, concat_axis=1, tiled=True)
    up_weight_grad = weight_rows[:, :gated_width] * grad_scale
    gate_weight_grad = weight_rows[:, gated_width:] * grad_scale
    return (input_grad[None], up_weight_grad, gate_weight_grad)


def solution(mesh):
    return jax.shard_map(
        on_device,
        mesh=mesh,
        in_specs=(
            P("dp", "sp", None),
            P("dp", "sp", None),
            P("dp", "sp", None),
            P("dp", "sp", None),
            P(),
            P("dp", None),
            P("dp", None),
            P(),
        ),
        out_specs=(P("dp", "sp", None), P("dp", None), P("dp", None)),
        check_vma=False,
    )
```

```python
import functools
import math

import jax
import jax.numpy as jnp
from jax import lax
from jax.experimental import pallas as pl
from jax.experimental.pallas import tpu as pltpu
from jax.sharding import PartitionSpec as P

GROUP_CH = 128
SPAN = 512
SEG = 64


norm_eps = 1e-05
grad_scale = 1.0 / 256.0
root_half = 1.0 / math.sqrt(2.0)
root_twopi = 1.0 / math.sqrt(2.0 * math.pi)


def gelu_value(preact):
    return 0.5 * preact * (1.0 + lax.erf(preact * root_half))


def gelu_slope(preact):
    return (
        0.5 * (1.0 + lax.erf(preact * root_half))
        + preact * jnp.exp(-0.5 * preact * preact) * root_twopi
    )


CHUNKS = 4
MESH = pl.DeviceIdType.MESH


def exchange_kernel(
    sizes, grads, columns, up_weight, gate_weight, sums, pieces,
    held, partial, x_arrived, x_sum, z_arrived, result,
    g_send, g_recv, x_send, x_recv, z_send, z_recv,
    az_send, az_recv, ax_send, ax_recv, r_send, r_recv,
):
    dps, xs, zs, chunks = sizes
    rows, width = grads.shape[0], grads.shape[1] // chunks
    share = partial.shape[3]
    f32 = jnp.float32
    dp_me = lax.axis_index("dp")
    sp_me = lax.axis_index("sp")
    x_me = lax.rem(sp_me, xs)
    z_me = lax.div(sp_me, xs)

    def at_dp(j):
        return {"dp": dp_me ^ j}

    def at_x(j):
        return {"sp": z_me * xs + (x_me ^ j)}

    def at_z(j):
        return {"sp": (z_me ^ j) * xs + x_me}

    def remote(src, dst, send, recv, where):
        return pltpu.make_async_remote_copy(
            src_ref=src, dst_ref=dst, send_sem=send, recv_sem=recv,
            device_id=where, device_id_type=MESH,
        )

    barrier = pltpu.get_barrier_semaphore()
    peers = [at_dp(j) for j in range(1, dps)]
    peers += [at_x(j) for j in range(1, xs)] + [at_z(j) for j in range(1, zs)]
    for peer in peers:
        pl.semaphore_signal(barrier, inc=1, device_id=peer, device_id_type=MESH)
    pl.semaphore_wait(barrier, len(peers))

    def grad_copy(k, j):
        if j == 1 or j % 2 == 0:
            return remote(
                grads.at[:, pl.ds(k * width, width)], held.at[k, j],
                g_send.at[k, j], g_recv.at[k, j], at_dp(j),
            )
        return remote(held.at[k, j - 1], held.at[k, j], g_send.at[k, j], g_recv.at[k, j], at_dp(1))

    def x_copy(k, j):
        return remote(
            partial.at[k, x_me ^ j], x_arrived.at[k, j], x_send.at[k, j], x_recv.at[k, j], at_x(j)
        )

    def z_copy(k, j):
        return remote(
            x_sum.at[k, z_me ^ j], z_arrived.at[k, j], z_send.at[k, j], z_recv.at[k, j], at_z(j)
        )

    def az_send_copy(k, j):
        block = sums.at[k, x_me, z_me]
        return remote(block, block, az_send.at[k, j], az_recv.at[k, j], at_z(j))

    def az_recv_copy(k, j):
        block = sums.at[k, x_me, z_me ^ j]
        return remote(block, block, az_send.at[k, j], az_recv.at[k, j], at_z(j))

    def ax_send_copy(k, j):
        block = sums.at[k, x_me]
        return remote(block, block, ax_send.at[k, j], ax_recv.at[k, j], at_x(j))

    def ax_recv_copy(k, j):
        block = sums.at[k, x_me ^ j]
        return remote(block, block, ax_send.at[k, j], ax_recv.at[k, j], at_x(j))

    def result_copy(j):
        return remote(result.at[j], pieces.at[dp_me], r_send.at[j], r_recv.at[j], at_dp(j))

    def result_recv_copy(j):
        return remote(result.at[j], pieces.at[dp_me ^ j], r_send.at[j], r_recv.at[j], at_dp(j))

    evens = range(2, dps, 2)
    odds = range(3, dps, 2)
    for k in range(chunks):
        for j in [*evens, 1]:
            grad_copy(k, j).start()
    for k in range(chunks):
        held[k, 0] = grads[:, k * width : (k + 1) * width]

    def first(k):
        for j in evens:
            grad_copy(k, j).wait_recv()
            grad_copy(k, j + 1).start()
        grad_copy(k, 1).wait_recv()
        for j in odds:
            grad_copy(k, j).wait_recv()
        tokens = held[k].reshape(dps * rows, width)
        part = jnp.dot(columns[...], tokens, preferred_element_type=f32)
        partial[k] = part.reshape(xs, zs, share, width).astype(jnp.bfloat16)
        for j in range(1, xs):
            x_copy(k, j).start()

    def second(k):
        total = partial[k, x_me].astype(f32)
        for j in range(1, xs):
            x_copy(k, j).wait_recv()
            total = total + x_arrived[k, j].astype(f32)
        x_sum[k] = total.astype(jnp.bfloat16)
        for j in range(1, zs):
            z_copy(k, j).start()

    def third(k):
        total = x_sum[k, z_me].astype(f32)
        for j in range(1, zs):
            z_copy(k, j).wait_recv()
            total = total + z_arrived[k, j].astype(f32)
        sums[k, x_me, z_me] = total.astype(jnp.bfloat16)
        for j in range(1, zs):
            az_send_copy(k, j).start()

    def fourth(k):
        for j in range(1, zs):
            az_recv_copy(k, j).wait_recv()
        for j in range(1, xs):
            ax_send_copy(k, j).start()

    def project():
        for j in [*range(1, dps), 0]:
            total = None
            for k in range(chunks):
                weight = up_weight if k < chunks // 2 else gate_weight
                at = k % (chunks // 2) * width
                term = lax.dot_general(
                    held[k, j], weight[:, at : at + width],
                    (((1,), (1,)), ((), ())), preferred_element_type=f32,
                )
                total = term if total is None else total + term
            if j == 0:
                pieces[dp_me] = total.astype(jnp.bfloat16)
            else:
                result[j] = total.astype(jnp.bfloat16)
                result_copy(j).start()

    for step in range(chunks + 3):
        for stage, lag in ((first, 0), (second, 1), (third, 2), (fourth, 3)):
            if 0 <= step - lag < chunks:
                stage(step - lag)
        if step == chunks - 1:
            project()
    for k in range(chunks):
        for j in range(1, xs):
            ax_recv_copy(k, j).wait_recv()
    for j in range(1, dps):
        result_recv_copy(j).wait_recv()
        result_copy(j).wait_send()
    for k in range(chunks):
        for j in range(1, dps):
            grad_copy(k, j).wait_send()
        for j in range(1, xs):
            x_copy(k, j).wait_send()
            ax_send_copy(k, j).wait_send()
        for j in range(1, zs):
            z_copy(k, j).wait_send()
            az_send_copy(k, j).wait_send()


def exchange(both_grads, columns, up_weight, gate_weight):
    dps = lax.axis_size("dp")
    sps = lax.axis_size("sp")
    xs = 2 ** ((sps.bit_length() - 1) // 2)
    zs = sps // xs
    rows, both_width = both_grads.shape
    width = both_width // CHUNKS
    own_columns = columns.shape[0]
    share = own_columns // sps
    bf16 = jnp.bfloat16
    vmem = pl.BlockSpec(memory_space=pltpu.VMEM)
    dma = pltpu.SemaphoreType.DMA
    return pl.pallas_call(
        functools.partial(exchange_kernel, (dps, xs, zs, CHUNKS)),
        out_shape=(
            jax.ShapeDtypeStruct((CHUNKS, xs, zs, share, width), bf16),
            jax.ShapeDtypeStruct((dps, rows, own_columns), bf16),
        ),
        in_specs=[vmem] * 4,
        out_specs=(vmem, vmem),
        scratch_shapes=[
            pltpu.VMEM((CHUNKS, dps, rows, width), bf16),
            pltpu.VMEM((CHUNKS, xs, zs, share, width), bf16),
            pltpu.VMEM((CHUNKS, xs, zs, share, width), bf16),
            pltpu.VMEM((CHUNKS, zs, share, width), bf16),
            pltpu.VMEM((CHUNKS, zs, share, width), bf16),
            pltpu.VMEM((dps, rows, own_columns), bf16),
        ]
        + [dma((CHUNKS, dps))] * 2
        + [dma((CHUNKS, xs))] * 2
        + [dma((CHUNKS, zs))] * 4
        + [dma((CHUNKS, xs))] * 2
        + [dma((dps,))] * 2,
        compiler_params=pltpu.CompilerParams(
            collective_id=0, has_side_effects=True, vmem_limit_bytes=60 * 1024 * 1024
        ),
    )(both_grads, columns, up_weight, gate_weight)


def on_device(inputs, up_pre, gate_pre, cotangent, norm_gain, up_weight, gate_weight, mix_weight):
    sequences, own_rows, gated_width = cotangent.shape
    model_width = inputs.shape[2]
    sp_count = lax.axis_size("sp")
    assert sequences == 1 and own_rows * 2 == SPAN
    groups = gated_width // GROUP_CH
    dp_count = lax.axis_size("dp")
    dp_me = lax.axis_index("dp")
    column_share = model_width // dp_count
    input_pieces = []
    for j in range(dp_count):
        piece = lax.dynamic_slice(
            inputs[0], (0, (dp_me ^ j) * column_share), (own_rows, column_share)
        )
        if j:
            piece = lax.ppermute(piece, "dp", [(i, i ^ j) for i in range(dp_count)])
        input_pieces.append(piece)
    columns = jnp.concatenate(input_pieces, axis=0).T
    up_float = up_pre[0].astype(jnp.float32)
    gate_float = gate_pre[0].astype(jnp.float32)
    grad_float = cotangent[0].astype(jnp.float32)
    gated_act = gelu_value(gate_float)
    centered = gated_act - jnp.mean(gated_act, axis=-1, keepdims=True)
    inverse_std = lax.rsqrt(jnp.mean(centered * centered, axis=-1, keepdims=True) + norm_eps)
    normed = centered * inverse_std
    mixer_in = (normed * norm_gain).astype(jnp.bfloat16)
    mixer_grad = (grad_float * gelu_value(up_float)).astype(jnp.bfloat16)
    half = lax.axis_index("sp") % 2
    arrived = lax.ppermute(
        jnp.where(half == 0, mixer_in, mixer_grad), "sp", [(i, i ^ 1) for i in range(sp_count)]
    )
    segment = jnp.arange(own_rows) // SEG
    own_block = lax.dynamic_slice(
        mix_weight, (0, half * own_rows, half * own_rows), (groups, own_rows, own_rows)
    )
    own_block = jnp.where(
        segment[None, :] <= segment[:, None], own_block, jnp.zeros_like(own_block)
    )
    cross_block = mix_weight[:, own_rows:, :own_rows]
    cross_block = jnp.where(half == 0, cross_block.transpose(0, 2, 1), cross_block)
    shape = (own_rows, groups, GROUP_CH)
    own_in = mixer_in.reshape(shape)
    own_grad = mixer_grad.reshape(shape)
    f32 = jnp.float32
    cross = jnp.einsum("gts,sgc->tgc", cross_block, arrived.reshape(shape), preferred_element_type=f32)
    spatial = jnp.einsum("gts,sgc->tgc", own_block, own_in, preferred_element_type=f32)
    back = jnp.einsum("gts,tgc->sgc", own_block, own_grad, preferred_element_type=f32)
    flat = (own_rows, gated_width)
    spatial = (spatial + jnp.where(half == 0, 0.0, cross)).astype(jnp.bfloat16).reshape(flat)
    back = (back + jnp.where(half == 0, cross, 0.0)).astype(jnp.bfloat16).reshape(flat)
    up_pre_grad = (grad_float * spatial.astype(f32) * gelu_slope(up_float)).astype(jnp.bfloat16)
    scaled = back.astype(f32) * norm_gain
    gated_grad = inverse_std * (
        scaled
        - jnp.mean(scaled, axis=-1, keepdims=True)
        - normed * jnp.mean(scaled * normed, axis=-1, keepdims=True)
    )
    gate_pre_grad = (gated_grad * gelu_slope(gate_float)).astype(jnp.bfloat16)
    both_grads = jnp.concatenate([up_pre_grad, gate_pre_grad], axis=1)
    sums, pieces = exchange(both_grads, columns, up_weight, gate_weight)
    input_grad = pieces.transpose(1, 0, 2).reshape(1, own_rows, model_width)
    half_chunks = CHUNKS // 2

    def rows_of(part):
        ordered = part.transpose(1, 2, 3, 0, 4).reshape(column_share, gated_width)
        return ordered.astype(f32) * grad_scale

    return (input_grad, rows_of(sums[:half_chunks]), rows_of(sums[half_chunks:]))


def solution(mesh):
    return jax.shard_map(
        on_device,
        mesh=mesh,
        in_specs=(
            P("dp", "sp", None),
            P("dp", "sp", None),
            P("dp", "sp", None),
            P("dp", "sp", None),
            P(),
            P("dp", None),
            P("dp", None),
            P(),
        ),
        out_specs=(P("dp", "sp", None), P("dp", None), P("dp", None)),
        check_vma=False,
    )
```

```python
import functools
import math

import jax
import jax.numpy as jnp
from jax import lax
from jax.experimental import pallas as pl
from jax.experimental.pallas import tpu as pltpu
from jax.sharding import PartitionSpec as P

GROUP_CH = 128
SPAN = 512
SEG = 64


norm_eps = 1e-05
grad_scale = 1.0 / 256.0
root_half = 1.0 / math.sqrt(2.0)
root_twopi = 1.0 / math.sqrt(2.0 * math.pi)


CHUNKS = 8
BAND = 16
MESH = pl.DeviceIdType.MESH


def exchange_kernel(
    sizes, inputs, up_pre, gate_pre, cotangent, gain, up_hbm, gate_hbm, mix_hbm, sums, pieces,
    up_weight, gate_weight, mix, own, other, normed_at, inverse_at, up_slope, gate_slope,
    spatial, back, col_arrived, columns,
    held, partial, x_arrived, x_sum, z_arrived, result,
    load, c_send, c_recv, p_send, p_recv,
    g_send, g_recv, x_send, x_recv, z_send, z_recv,
    az_send, az_recv, ax_send, ax_recv, r_send, r_recv,
):
    dps, xs, zs, chunks = sizes
    rows, gated = own.shape[1:]
    width = 2 * gated // chunks
    column_share = columns.shape[0]
    share = partial.shape[3]
    f32 = jnp.float32
    dp_me = lax.axis_index("dp")
    sp_me = lax.axis_index("sp")
    x_me = lax.rem(sp_me, xs)
    z_me = lax.div(sp_me, xs)

    def at_dp(j):
        return {"dp": dp_me ^ j}

    def at_x(j):
        return {"sp": z_me * xs + (x_me ^ j)}

    def at_z(j):
        return {"sp": (z_me ^ j) * xs + x_me}

    def remote(src, dst, send, recv, where):
        return pltpu.make_async_remote_copy(
            src_ref=src, dst_ref=dst, send_sem=send, recv_sem=recv,
            device_id=where, device_id_type=MESH,
        )

    loads = [
        pltpu.make_async_copy(mix_hbm, mix, load.at[0]),
        pltpu.make_async_copy(up_hbm, up_weight, load.at[1]),
        pltpu.make_async_copy(gate_hbm, gate_weight, load.at[2]),
    ]
    for copy in loads:
        copy.start()
    barrier = pltpu.get_barrier_semaphore()
    peers = [at_dp(j) for j in range(1, dps)]
    peers += [at_x(j) for j in range(1, xs)] + [at_z(j) for j in range(1, zs)]
    for peer in peers:
        pl.semaphore_signal(barrier, inc=1, device_id=peer, device_id_type=MESH)
    pl.semaphore_wait(barrier, len(peers))

    def grad_copy(k, j):
        if j == 1 or j % 2 == 0:
            return remote(
                held.at[k, 0], held.at[k, j],
                g_send.at[k, j], g_recv.at[k, j], at_dp(j),
            )
        return remote(held.at[k, j - 1], held.at[k, j], g_send.at[k, j], g_recv.at[k, j], at_dp(1))

    def x_copy(k, j):
        return remote(
            partial.at[k, x_me ^ j], x_arrived.at[k, j], x_send.at[k, j], x_recv.at[k, j], at_x(j)
        )

    def z_copy(k, j):
        return remote(
            x_sum.at[k, z_me ^ j], z_arrived.at[k, j], z_send.at[k, j], z_recv.at[k, j], at_z(j)
        )

    def az_send_copy(k, j):
        block = sums.at[x_me, z_me, :, pl.ds(k * width, width)]
        return remote(block, block, az_send.at[k, j], az_recv.at[k, j], at_z(j))

    def az_recv_copy(k, j):
        block = sums.at[x_me, z_me ^ j, :, pl.ds(k * width, width)]
        return remote(block, block, az_send.at[k, j], az_recv.at[k, j], at_z(j))

    def ax_send_copy(k, j):
        block = sums.at[x_me, :, :, pl.ds(k * width, width)]
        return remote(block, block, ax_send.at[k, j], ax_recv.at[k, j], at_x(j))

    def ax_recv_copy(k, j):
        block = sums.at[x_me ^ j, :, :, pl.ds(k * width, width)]
        return remote(block, block, ax_send.at[k, j], ax_recv.at[k, j], at_x(j))

    def columns_of(who):
        return pl.ds(pl.multiple_of(who * column_share, column_share), column_share)

    def column_copy(j):
        return remote(
            inputs.at[:, columns_of(dp_me ^ j)], col_arrived.at[j],
            c_send.at[j], c_recv.at[j], at_dp(j),
        )

    half = lax.rem(sp_me, 2)
    part_rows = rows // 2

    def pair_copy(b):
        span = pl.ds(b * part_rows, part_rows)
        return remote(own.at[half, span], other.at[span], p_send.at[b], p_recv.at[b], at_x(1))

    def result_copy(j):
        return remote(result.at[j], pieces.at[:, columns_of(dp_me)], r_send.at[j], r_recv.at[j], at_dp(j))

    def result_recv_copy(j):
        return remote(result.at[j], pieces.at[:, columns_of(dp_me ^ j)], r_send.at[j], r_recv.at[j], at_dp(j))

    evens = range(2, dps, 2)
    odds = range(3, dps, 2)
    for j in range(1, dps):
        column_copy(j).start()

    def slopes(band):
        at = pl.ds(pl.multiple_of(band * BAND, BAND), BAND)
        gate = gate_pre[at, :].astype(f32)
        cdf = 0.5 * (1.0 + lax.erf(gate * root_half))
        gate_slope[at, :] = cdf + gate * jnp.exp(-0.5 * gate * gate) * root_twopi
        act = gate * cdf
        centered = act - jnp.mean(act, axis=-1, keepdims=True)
        inverse = lax.rsqrt(jnp.mean(centered * centered, axis=-1, keepdims=True) + norm_eps)
        normed = centered * inverse
        normed_at[at, :] = normed
        inverse_at[at, :] = jnp.broadcast_to(inverse, (BAND, 128))
        own[0, at, :] = (normed * gain[...]).astype(jnp.bfloat16)
        up = up_pre[at, :].astype(f32)
        grad = cotangent[at, :].astype(f32)
        cdf = 0.5 * (1.0 + lax.erf(up * root_half))
        up_slope[at, :] = grad * (cdf + up * jnp.exp(-0.5 * up * up) * root_twopi)
        own[1, at, :] = (grad * (up * cdf)).astype(jnp.bfloat16)

    bands = part_rows // BAND
    for b in range(2):
        pl.loop(b * bands, (b + 1) * bands)(slopes)
        pair_copy(b).start()

    loads[0].wait()
    own_rows = pl.ds(pl.multiple_of(half * rows, rows), rows)
    row_segment = lax.broadcasted_iota(jnp.int32, (rows, rows), 0) // SEG
    column_segment = lax.broadcasted_iota(jnp.int32, (rows, rows), 1) // SEG
    seen = column_segment <= row_segment
    groups = mix.shape[0]

    def group_dot(weight, value, dim):
        return lax.dot_general(
            weight, value, (((dim,), (0,)), ((), ())), preferred_element_type=f32
        )

    for g in range(groups):
        lanes = slice(g * GROUP_CH, (g + 1) * GROUP_CH)
        block = mix[g, own_rows, own_rows]
        block = jnp.where(seen, block, jnp.zeros_like(block))
        spatial[:, lanes] = group_dot(block, own[0, :, lanes], 1)
        back[:, lanes] = group_dot(block, own[1, :, lanes], 0)
    for b in range(2):
        pair_copy(b).wait_recv()

    @pl.when(half == 1)
    def _():
        for g in range(groups):
            lanes = slice(g * GROUP_CH, (g + 1) * GROUP_CH)
            spatial[:, lanes] += group_dot(mix[g, rows:, :rows], other[:, lanes], 1)

    @pl.when(half == 0)
    def _():
        for g in range(groups):
            lanes = slice(g * GROUP_CH, (g + 1) * GROUP_CH)
            back[:, lanes] += group_dot(mix[g, rows:, :rows], other[:, lanes], 0)

    def up_band(band):
        at = pl.ds(pl.multiple_of(band * BAND, BAND), BAND)
        mixed = spatial[at, :].astype(jnp.bfloat16).astype(f32)
        grad = (mixed * up_slope[at, :]).astype(jnp.bfloat16)
        for k in range(chunks // 2):
            held[k, 0, at, :] = grad[:, k * width : (k + 1) * width]

    def gate_band(band):
        at = pl.ds(pl.multiple_of(band * BAND, BAND), BAND)
        scaled = back[at, :].astype(jnp.bfloat16).astype(f32) * gain[...]
        normed = normed_at[at, :]
        grad = inverse_at[at, 0:1] * (
            scaled
            - jnp.mean(scaled, axis=-1, keepdims=True)
            - normed * jnp.mean(scaled * normed, axis=-1, keepdims=True)
        )
        grad = (grad * gate_slope[at, :]).astype(jnp.bfloat16)
        for k in range(chunks // 2):
            held[chunks // 2 + k, 0, at, :] = grad[:, k * width : (k + 1) * width]

    pl.loop(0, rows // BAND)(up_band)
    for k in range(chunks // 2):
        for j in [*evens, 1]:
            grad_copy(k, j).start()
    pl.loop(0, rows // BAND)(gate_band)
    for k in range(chunks // 2, chunks):
        for j in [*evens, 1]:
            grad_copy(k, j).start()
    columns[:, :rows] = inputs[:, columns_of(dp_me)].T
    for j in range(1, dps):
        column_copy(j).wait_recv()
        columns[:, j * rows : (j + 1) * rows] = col_arrived[j].T

    def first(k):
        for j in evens:
            grad_copy(k, j).wait_recv()
            grad_copy(k, j + 1).start()
        grad_copy(k, 1).wait_recv()
        for j in odds:
            grad_copy(k, j).wait_recv()
        tokens = held[k].reshape(dps * rows, width)
        part = jnp.dot(columns[...], tokens, preferred_element_type=f32)
        partial[k] = part.reshape(xs, zs, share, width).astype(jnp.bfloat16)
        for j in range(1, xs):
            x_copy(k, j).start()

    def second(k):
        total = partial[k, x_me].astype(f32)
        for j in range(1, xs):
            x_copy(k, j).wait_recv()
            total = total + x_arrived[k, j].astype(f32)
        x_sum[k] = total.astype(jnp.bfloat16)
        for j in range(1, zs):
            z_copy(k, j).start()

    def third(k):
        total = x_sum[k, z_me].astype(f32)
        for j in range(1, zs):
            z_copy(k, j).wait_recv()
            total = total + z_arrived[k, j].astype(f32)
        sums[x_me, z_me, :, k * width : (k + 1) * width] = total.astype(jnp.bfloat16)
        for j in range(1, zs):
            az_send_copy(k, j).start()

    def fourth(k):
        for j in range(1, zs):
            az_recv_copy(k, j).wait_recv()
        for j in range(1, xs):
            ax_send_copy(k, j).start()

    def project():
        loads[1].wait()
        loads[2].wait()
        for j in [*range(1, dps), 0]:
            total = None
            for k in range(chunks):
                weight = up_weight if k < chunks // 2 else gate_weight
                at = k % (chunks // 2) * width
                term = lax.dot_general(
                    held[k, j], weight[:, at : at + width],
                    (((1,), (1,)), ((), ())), preferred_element_type=f32,
                )
                total = term if total is None else total + term
            if j == 0:
                pieces[:, columns_of(dp_me)] = total.astype(jnp.bfloat16)
            else:
                result[j] = total.astype(jnp.bfloat16)
                result_copy(j).start()

    for step in range(chunks + 3):
        for stage, lag in ((first, 0), (second, 1), (third, 2), (fourth, 3)):
            if 0 <= step - lag < chunks:
                stage(step - lag)
        if step == chunks - 1:
            project()
    for k in range(chunks):
        for j in range(1, xs):
            ax_recv_copy(k, j).wait_recv()
    for b in range(2):
        pair_copy(b).wait_send()
    for j in range(1, dps):
        column_copy(j).wait_send()
        result_recv_copy(j).wait_recv()
        result_copy(j).wait_send()
    for k in range(chunks):
        for j in range(1, dps):
            grad_copy(k, j).wait_send()
        for j in range(1, xs):
            x_copy(k, j).wait_send()
            ax_send_copy(k, j).wait_send()
        for j in range(1, zs):
            z_copy(k, j).wait_send()
            az_send_copy(k, j).wait_send()


def on_device(inputs, up_pre, gate_pre, cotangent, norm_gain, up_weight, gate_weight, mix_weight):
    sequences, rows, gated = cotangent.shape
    model_width = inputs.shape[2]
    assert sequences == 1 and rows * 2 == SPAN
    dps = lax.axis_size("dp")
    sps = lax.axis_size("sp")
    xs = 2 ** ((sps.bit_length() - 1) // 2)
    zs = sps // xs
    width = 2 * gated // CHUNKS
    own_columns = model_width // dps
    share = own_columns // sps
    bf16 = jnp.bfloat16
    f32 = jnp.float32
    vmem = pl.BlockSpec(memory_space=pltpu.VMEM)
    hbm = pl.BlockSpec(memory_space=pl.ANY)
    dma = pltpu.SemaphoreType.DMA
    flat = (rows, gated)
    sums, input_grad = pl.pallas_call(
        functools.partial(exchange_kernel, (dps, xs, zs, CHUNKS)),
        out_shape=(
            jax.ShapeDtypeStruct((xs, zs, share, 2 * gated), bf16),
            jax.ShapeDtypeStruct((rows, model_width), bf16),
        ),
        in_specs=[vmem] * 5 + [hbm] * 3,
        out_specs=(vmem, vmem),
        scratch_shapes=[
            pltpu.VMEM(up_weight.shape, bf16),
            pltpu.VMEM(gate_weight.shape, bf16),
            pltpu.VMEM(mix_weight.shape, bf16),
            pltpu.VMEM((2, *flat), bf16),
            pltpu.VMEM(flat, bf16),
            pltpu.VMEM(flat, f32),
            pltpu.VMEM((rows, 128), f32),
            pltpu.VMEM(flat, f32),
            pltpu.VMEM(flat, f32),
            pltpu.VMEM(flat, f32),
            pltpu.VMEM(flat, f32),
            pltpu.VMEM((dps, rows, own_columns), bf16),
            pltpu.VMEM((own_columns, dps * rows), bf16),
            pltpu.VMEM((CHUNKS, dps, rows, width), bf16),
            pltpu.VMEM((CHUNKS, xs, zs, share, width), bf16),
            pltpu.VMEM((CHUNKS, xs, zs, share, width), bf16),
            pltpu.VMEM((CHUNKS, zs, share, width), bf16),
            pltpu.VMEM((CHUNKS, zs, share, width), bf16),
            pltpu.VMEM((dps, rows, own_columns), bf16),
        ]
        + [dma((3,))]
        + [dma((dps,))] * 2
        + [dma((2,))] * 2
        + [dma((CHUNKS, dps))] * 2
        + [dma((CHUNKS, xs))] * 2
        + [dma((CHUNKS, zs))] * 4
        + [dma((CHUNKS, xs))] * 2
        + [dma((dps,))] * 2,
        compiler_params=pltpu.CompilerParams(
            collective_id=0, has_side_effects=True, vmem_limit_bytes=60 * 1024 * 1024
        ),
    )(
        inputs[0], up_pre[0], gate_pre[0], cotangent[0], norm_gain[None],
        up_weight, gate_weight, mix_weight,
    )
    weight_rows = sums.reshape(own_columns, 2 * gated).astype(f32) * grad_scale
    return (input_grad[None], weight_rows[:, :gated], weight_rows[:, gated:])


def solution(mesh):
    return jax.shard_map(
        on_device,
        mesh=mesh,
        in_specs=(
            P("dp", "sp", None),
            P("dp", "sp", None),
            P("dp", "sp", None),
            P("dp", "sp", None),
            P(),
            P("dp", None),
            P("dp", None),
            P(),
        ),
        out_specs=(P("dp", "sp", None), P("dp", None), P("dp", None)),
        check_vma=False,
    )
```

```python
import functools
import math

import jax
import jax.numpy as jnp
from jax import lax
from jax.experimental import pallas as pl
from jax.experimental.pallas import tpu as pltpu
from jax.sharding import PartitionSpec as P

GROUP_CH = 128
SPAN = 512
SEG = 64


norm_eps = 1e-05
grad_scale = 1.0 / 256.0
root_half = 1.0 / math.sqrt(2.0)
root_twopi = 1.0 / math.sqrt(2.0 * math.pi)


CHUNKS = 8
BAND = 16
MESH = pl.DeviceIdType.MESH


def exchange_kernel(
    sizes, inputs, up_pre, gate_pre, cotangent, gain, up_hbm, gate_hbm, mix_hbm, sums, pieces,
    up_weight, gate_weight, mix, own, other, normed_at, inverse_at, up_slope, gate_slope,
    spatial, back, col_arrived, columns,
    held, partial, x_arrived, x_sum, z_arrived, result,
    load, c_send, c_recv, p_send, p_recv,
    g_send, g_recv, x_send, x_recv, z_send, z_recv,
    az_send, az_recv, ax_send, ax_recv, r_send, r_recv,
):
    dps, xs, zs, chunks = sizes
    rows, gated = own.shape[1:]
    width = 2 * gated // chunks
    column_share = columns.shape[0]
    share = partial.shape[3]
    f32 = jnp.float32
    dp_me = lax.axis_index("dp")
    sp_me = lax.axis_index("sp")
    x_me = lax.rem(sp_me, xs)
    z_me = lax.div(sp_me, xs)

    def lanes_of(k):
        return pl.ds(pl.multiple_of(k * width, width), width)

    def order(k):
        return lax.rem(k + lax.rem(sp_me, 2) * (chunks // 2), chunks)

    def at_dp(j):
        return {"dp": dp_me ^ j}

    def at_x(j):
        return {"sp": z_me * xs + (x_me ^ j)}

    def at_z(j):
        return {"sp": (z_me ^ j) * xs + x_me}

    def remote(src, dst, send, recv, where):
        return pltpu.make_async_remote_copy(
            src_ref=src, dst_ref=dst, send_sem=send, recv_sem=recv,
            device_id=where, device_id_type=MESH,
        )

    loads = [
        pltpu.make_async_copy(mix_hbm, mix, load.at[0]),
        pltpu.make_async_copy(up_hbm, up_weight, load.at[1]),
        pltpu.make_async_copy(gate_hbm, gate_weight, load.at[2]),
    ]
    for copy in loads:
        copy.start()
    barrier = pltpu.get_barrier_semaphore()
    peers = [at_dp(j) for j in range(1, dps)]
    peers += [at_x(j) for j in range(1, xs)] + [at_z(j) for j in range(1, zs)]
    for peer in peers:
        pl.semaphore_signal(barrier, inc=1, device_id=peer, device_id_type=MESH)
    pl.semaphore_wait(barrier, len(peers))

    def grad_copy(k, j):
        if j == 1 or j % 2 == 0:
            return remote(
                held.at[k, 0], held.at[k, j],
                g_send.at[k, j], g_recv.at[k, j], at_dp(j),
            )
        return remote(held.at[k, j - 1], held.at[k, j], g_send.at[k, j], g_recv.at[k, j], at_dp(1))

    def x_copy(k, j):
        return remote(
            partial.at[k, x_me ^ j], x_arrived.at[k, j], x_send.at[k, j], x_recv.at[k, j], at_x(j)
        )

    def z_copy(k, j):
        return remote(
            x_sum.at[k, z_me ^ j], z_arrived.at[k, j], z_send.at[k, j], z_recv.at[k, j], at_z(j)
        )

    def az_send_copy(k, j):
        block = sums.at[x_me, z_me, :, lanes_of(k)]
        return remote(block, block, az_send.at[k, j], az_recv.at[k, j], at_z(j))

    def az_recv_copy(k, j):
        block = sums.at[x_me, z_me ^ j, :, lanes_of(k)]
        return remote(block, block, az_send.at[k, j], az_recv.at[k, j], at_z(j))

    def ax_send_copy(k, j):
        block = sums.at[x_me, :, :, lanes_of(k)]
        return remote(block, block, ax_send.at[k, j], ax_recv.at[k, j], at_x(j))

    def ax_recv_copy(k, j):
        block = sums.at[x_me ^ j, :, :, lanes_of(k)]
        return remote(block, block, ax_send.at[k, j], ax_recv.at[k, j], at_x(j))

    def columns_of(who):
        return pl.ds(pl.multiple_of(who * column_share, column_share), column_share)

    def column_copy(j):
        return remote(
            inputs.at[:, columns_of(dp_me ^ j)], col_arrived.at[j],
            c_send.at[j], c_recv.at[j], at_dp(j),
        )

    half = lax.rem(sp_me, 2)
    part_rows = rows // 2

    def pair_copy(b):
        span = pl.ds(b * part_rows, part_rows)
        return remote(own.at[half, span], other.at[span], p_send.at[b], p_recv.at[b], at_x(1))

    def result_copy(j):
        return remote(result.at[j], pieces.at[:, columns_of(dp_me)], r_send.at[j], r_recv.at[j], at_dp(j))

    def result_recv_copy(j):
        return remote(result.at[j], pieces.at[:, columns_of(dp_me ^ j)], r_send.at[j], r_recv.at[j], at_dp(j))

    evens = range(2, dps, 2)
    odds = range(3, dps, 2)
    for j in range(1, dps):
        column_copy(j).start()

    def slopes(band):
        at = pl.ds(pl.multiple_of(band * BAND, BAND), BAND)
        gate = gate_pre[at, :].astype(f32)
        cdf = 0.5 * (1.0 + lax.erf(gate * root_half))
        gate_slope[at, :] = cdf + gate * jnp.exp(-0.5 * gate * gate) * root_twopi
        act = gate * cdf
        centered = act - jnp.mean(act, axis=-1, keepdims=True)
        inverse = lax.rsqrt(jnp.mean(centered * centered, axis=-1, keepdims=True) + norm_eps)
        normed = centered * inverse
        normed_at[at, :] = normed
        inverse_at[at, :] = jnp.broadcast_to(inverse, (BAND, 128))
        own[0, at, :] = (normed * gain[...]).astype(jnp.bfloat16)
        up = up_pre[at, :].astype(f32)
        grad = cotangent[at, :].astype(f32)
        cdf = 0.5 * (1.0 + lax.erf(up * root_half))
        up_slope[at, :] = grad * (cdf + up * jnp.exp(-0.5 * up * up) * root_twopi)
        own[1, at, :] = (grad * (up * cdf)).astype(jnp.bfloat16)

    bands = part_rows // BAND
    for b in range(2):
        pl.loop(b * bands, (b + 1) * bands)(slopes)
        pair_copy(b).start()

    loads[0].wait()
    own_rows = pl.ds(pl.multiple_of(half * rows, rows), rows)
    row_segment = lax.broadcasted_iota(jnp.int32, (rows, rows), 0) // SEG
    column_segment = lax.broadcasted_iota(jnp.int32, (rows, rows), 1) // SEG
    seen = column_segment <= row_segment
    groups = mix.shape[0]

    def group_dot(weight, value, dim):
        return lax.dot_general(
            weight, value, (((dim,), (0,)), ((), ())), preferred_element_type=f32
        )

    for g in range(groups):
        lanes = slice(g * GROUP_CH, (g + 1) * GROUP_CH)
        block = mix[g, own_rows, own_rows]
        block = jnp.where(seen, block, jnp.zeros_like(block))
        spatial[:, lanes] = group_dot(block, own[0, :, lanes], 1)
        back[:, lanes] = group_dot(block, own[1, :, lanes], 0)
    def send_grads(ks):
        for k in ks:
            for j in [*evens, 1]:
                grad_copy(order(k), j).start()

    def up_band(band):
        at = pl.ds(pl.multiple_of(band * BAND, BAND), BAND)
        mixed = spatial[at, :].astype(jnp.bfloat16).astype(f32)
        grad = (mixed * up_slope[at, :]).astype(jnp.bfloat16)
        for k in range(chunks // 2):
            held[k, 0, at, :] = grad[:, k * width : (k + 1) * width]

    def gate_band(band):
        at = pl.ds(pl.multiple_of(band * BAND, BAND), BAND)
        scaled = back[at, :].astype(jnp.bfloat16).astype(f32) * gain[...]
        normed = normed_at[at, :]
        grad = inverse_at[at, 0:1] * (
            scaled
            - jnp.mean(scaled, axis=-1, keepdims=True)
            - normed * jnp.mean(scaled * normed, axis=-1, keepdims=True)
        )
        grad = (grad * gate_slope[at, :]).astype(jnp.bfloat16)
        for k in range(chunks // 2):
            held[chunks // 2 + k, 0, at, :] = grad[:, k * width : (k + 1) * width]

    @pl.when(half == 0)
    def _():
        pl.loop(0, rows // BAND)(up_band)

    @pl.when(half == 1)
    def _():
        pl.loop(0, rows // BAND)(gate_band)

    send_grads(range(chunks // 2))
    for b in range(2):
        pair_copy(b).wait_recv()

    @pl.when(half == 1)
    def _():
        for g in range(groups):
            lanes = slice(g * GROUP_CH, (g + 1) * GROUP_CH)
            spatial[:, lanes] += group_dot(mix[g, rows:, :rows], other[:, lanes], 1)
        pl.loop(0, rows // BAND)(up_band)

    @pl.when(half == 0)
    def _():
        for g in range(groups):
            lanes = slice(g * GROUP_CH, (g + 1) * GROUP_CH)
            back[:, lanes] += group_dot(mix[g, rows:, :rows], other[:, lanes], 0)
        pl.loop(0, rows // BAND)(gate_band)

    send_grads(range(chunks // 2, chunks))
    columns[:, :rows] = inputs[:, columns_of(dp_me)].T
    for j in range(1, dps):
        column_copy(j).wait_recv()
        columns[:, j * rows : (j + 1) * rows] = col_arrived[j].T

    def first(k):
        for j in evens:
            grad_copy(k, j).wait_recv()
            grad_copy(k, j + 1).start()
        grad_copy(k, 1).wait_recv()
        for j in odds:
            grad_copy(k, j).wait_recv()
        tokens = held[k].reshape(dps * rows, width)
        part = jnp.dot(columns[...], tokens, preferred_element_type=f32)
        partial[k] = part.reshape(xs, zs, share, width).astype(jnp.bfloat16)
        for j in range(1, xs):
            x_copy(k, j).start()

    def second(k):
        total = partial[k, x_me].astype(f32)
        for j in range(1, xs):
            x_copy(k, j).wait_recv()
            total = total + x_arrived[k, j].astype(f32)
        x_sum[k] = total.astype(jnp.bfloat16)
        for j in range(1, zs):
            z_copy(k, j).start()

    def third(k):
        total = x_sum[k, z_me].astype(f32)
        for j in range(1, zs):
            z_copy(k, j).wait_recv()
            total = total + z_arrived[k, j].astype(f32)
        sums[x_me, z_me, :, lanes_of(k)] = total.astype(jnp.bfloat16)
        for j in range(1, zs):
            az_send_copy(k, j).start()

    def fourth(k):
        for j in range(1, zs):
            az_recv_copy(k, j).wait_recv()
        for j in range(1, xs):
            ax_send_copy(k, j).start()

    def project():
        loads[1].wait()
        loads[2].wait()
        for j in [*range(1, dps), 0]:
            total = None
            for k in range(chunks):
                weight = up_weight if k < chunks // 2 else gate_weight
                at = k % (chunks // 2) * width
                term = lax.dot_general(
                    held[k, j], weight[:, at : at + width],
                    (((1,), (1,)), ((), ())), preferred_element_type=f32,
                )
                total = term if total is None else total + term
            if j == 0:
                pieces[:, columns_of(dp_me)] = total.astype(jnp.bfloat16)
            else:
                result[j] = total.astype(jnp.bfloat16)
                result_copy(j).start()

    middle = chunks // 2
    for step in range(chunks + 2):
        if step < chunks:
            first(order(step))
        if middle <= step < chunks:
            second(order(step))
        if middle < step <= chunks:
            second(order(step - 1 - middle))
            third(order(step - 1))
        if middle + 1 < step:
            third(order(step - 2 - middle))
            fourth(order(step - 2))
        if step == chunks - 1:
            project()
        if middle + 2 < step:
            fourth(order(step - 3 - middle))
    fourth(order(middle - 1))
    for k in range(chunks):
        for j in range(1, xs):
            ax_recv_copy(k, j).wait_recv()
    for b in range(2):
        pair_copy(b).wait_send()
    for j in range(1, dps):
        column_copy(j).wait_send()
        result_recv_copy(j).wait_recv()
        result_copy(j).wait_send()
    for k in range(chunks):
        for j in range(1, dps):
            grad_copy(k, j).wait_send()
        for j in range(1, xs):
            x_copy(k, j).wait_send()
            ax_send_copy(k, j).wait_send()
        for j in range(1, zs):
            z_copy(k, j).wait_send()
            az_send_copy(k, j).wait_send()


def on_device(inputs, up_pre, gate_pre, cotangent, norm_gain, up_weight, gate_weight, mix_weight):
    sequences, rows, gated = cotangent.shape
    model_width = inputs.shape[2]
    assert sequences == 1 and rows * 2 == SPAN
    dps = lax.axis_size("dp")
    sps = lax.axis_size("sp")
    xs = 2 ** ((sps.bit_length() - 1) // 2)
    zs = sps // xs
    width = 2 * gated // CHUNKS
    own_columns = model_width // dps
    share = own_columns // sps
    bf16 = jnp.bfloat16
    f32 = jnp.float32
    vmem = pl.BlockSpec(memory_space=pltpu.VMEM)
    hbm = pl.BlockSpec(memory_space=pl.ANY)
    dma = pltpu.SemaphoreType.DMA
    flat = (rows, gated)
    sums, input_grad = pl.pallas_call(
        functools.partial(exchange_kernel, (dps, xs, zs, CHUNKS)),
        out_shape=(
            jax.ShapeDtypeStruct((xs, zs, share, 2 * gated), bf16),
            jax.ShapeDtypeStruct((rows, model_width), bf16),
        ),
        in_specs=[vmem] * 5 + [hbm] * 3,
        out_specs=(vmem, vmem),
        scratch_shapes=[
            pltpu.VMEM(up_weight.shape, bf16),
            pltpu.VMEM(gate_weight.shape, bf16),
            pltpu.VMEM(mix_weight.shape, bf16),
            pltpu.VMEM((2, *flat), bf16),
            pltpu.VMEM(flat, bf16),
            pltpu.VMEM(flat, f32),
            pltpu.VMEM((rows, 128), f32),
            pltpu.VMEM(flat, f32),
            pltpu.VMEM(flat, f32),
            pltpu.VMEM(flat, f32),
            pltpu.VMEM(flat, f32),
            pltpu.VMEM((dps, rows, own_columns), bf16),
            pltpu.VMEM((own_columns, dps * rows), bf16),
            pltpu.VMEM((CHUNKS, dps, rows, width), bf16),
            pltpu.VMEM((CHUNKS, xs, zs, share, width), bf16),
            pltpu.VMEM((CHUNKS, xs, zs, share, width), bf16),
            pltpu.VMEM((CHUNKS, zs, share, width), bf16),
            pltpu.VMEM((CHUNKS, zs, share, width), bf16),
            pltpu.VMEM((dps, rows, own_columns), bf16),
        ]
        + [dma((3,))]
        + [dma((dps,))] * 2
        + [dma((2,))] * 2
        + [dma((CHUNKS, dps))] * 2
        + [dma((CHUNKS, xs))] * 2
        + [dma((CHUNKS, zs))] * 4
        + [dma((CHUNKS, xs))] * 2
        + [dma((dps,))] * 2,
        compiler_params=pltpu.CompilerParams(
            collective_id=0, has_side_effects=True, vmem_limit_bytes=60 * 1024 * 1024
        ),
    )(
        inputs[0], up_pre[0], gate_pre[0], cotangent[0], norm_gain[None],
        up_weight, gate_weight, mix_weight,
    )
    weight_rows = sums.reshape(own_columns, 2 * gated).astype(f32) * grad_scale
    return (input_grad[None], weight_rows[:, :gated], weight_rows[:, gated:])


def solution(mesh):
    return jax.shard_map(
        on_device,
        mesh=mesh,
        in_specs=(
            P("dp", "sp", None),
            P("dp", "sp", None),
            P("dp", "sp", None),
            P("dp", "sp", None),
            P(),
            P("dp", None),
            P("dp", None),
            P(),
        ),
        out_specs=(P("dp", "sp", None), P("dp", None), P("dp", None)),
        check_vma=False,
    )
```
